32 devices in a mesh: vp: 4 (over y, x), dp: 8 (over z, core).
Axes of the slice: x: 2, y: 2, z: 4, core: 2. Of those that a mesh axis runs over, the one named last changes fastest.
Arguments:
- hidden_act: bfloat16 [4096, 8192], P('dp', 'vp'), may hold values from 0 to 36
- down_weight: bfloat16 [8192, 2048], P('vp'), may hold values from -0.0625 to 0.0625
- residual: bfloat16 [4096, 2048], P(('dp', 'vp')), may hold values from -300 to 300
- post_gain: float32 [2048], replicated, may hold values from 0.1 to 1.9
- final_gain: float32 [2048], replicated, may hold values from 0.1 to 1.9
- vocab: bfloat16 [2048, 32768], P(None, 'vp'), may hold values from -0.33 to 0.33
- vocab_bias: float32 [32768], P('vp'), may hold values from -2.5 to 2.5
- target_ids: int32 [4096, 4], P('dp'), may hold values from 0 to 32767
- target_weights: float32 [4096, 4], P('dp'), may hold values from 0 to 1, as said below
Outputs:
- losses: float32 [4096], P(('dp', 'vp'))
- stream_grad: float32 [4096, 2048], P(('dp', 'vp'))
- vocab_grad: float32 [2048, 32768], P('dp', 'vp')
The draws below stay inside these ranges and needn't reach their ends.
Inputs may be any that keep to these rules, and one draw needn't show every extreme that they name: `target_weights`: the 4 weights of a token add up to one.
All inputs are finite; a program needn't handle non-finite values.
Results may differ from the reference program's by a relative error of at most 0.01225.
Values may be sent and summed in bfloat16 or wider, within the bound.
A program may use at most 192 MiB of HBM per device.

```python
import math
import jax
import jax.numpy as jnp
import numpy as np
from jax import lax

D = 2048
FF = 8192
V = 32768
TOPK = 4
TOK_GRP = 512
TOKENS = 4096
N_VP = 4
N_DP = 8


def spike_signs(key):
    return (jax.random.randint(jax.random.fold_in(key, 4242), (D,), 0, 2) * 2 - 1).astype(jnp.float32)


def draw_hidden_act(key, part):
    values = jax.random.normal(jax.random.fold_in(key, 41), (TOKENS, FF), jnp.float32)
    values = jnp.clip(values, -6.0, 6.0)
    positive = jnp.maximum(values, 0.0)
    return (positive * positive).astype(jnp.bfloat16)


def draw_residual(key, part):
    values = jnp.clip(jax.random.normal(jax.random.fold_in(key, 11), (TOKENS, D), jnp.float32), -6.0, 6.0)
    marked = (jnp.arange(TOKENS) % 61 == 3)[:, None]
    values = jnp.where(marked, 300.0 * spike_signs(key)[None, :], values)
    return values.astype(jnp.bfloat16)


def draw_vocab(key, part):
    values = 0.055 * jnp.clip(jax.random.normal(jax.random.fold_in(key, 21), (D, V), jnp.float32), -6.0, 6.0)
    marked = (jnp.arange(V) % 509 == 7)[None, :]
    values = jnp.where(marked, 256.0 / D * spike_signs(key)[:, None], values)
    return values.astype(jnp.bfloat16)


def draw_vocab_bias(key, part):
    offsets = jax.random.uniform(jax.random.fold_in(key, 31), (N_VP,), jnp.float32, -1.5, 1.5)
    shard_of = jnp.arange(V) // (V // N_VP)
    values = 0.5 * jnp.clip(jax.random.normal(jax.random.fold_in(key, 32), (V,), jnp.float32), -2.0, 2.0)
    return offsets[shard_of] + values


def draw_target_weights(key, part):
    logits = 1.5 * jax.random.normal(jax.random.fold_in(key, 52), (TOKENS, TOPK), jnp.float32)
    return jax.nn.softmax(logits, axis=-1)


def place_ends(entries, key, smallest, top_value):
    spot = [jax.random.randint(jax.random.fold_in(key, axis), (), 0, length) for axis, length in enumerate(entries.shape)]
    widest = entries.shape.index(max(entries.shape))
    next_to = spot[:widest] + [(spot[widest] + 1) % entries.shape[widest]] + spot[widest + 1:]
    return entries.at[tuple(spot)].set(smallest).at[tuple(next_to)].set(top_value)


def steps_of(own_key, extent, cuts, low, largest):
    factor_of = 1.0
    for axis_at, parts in cuts:
        draws = jax.random.uniform(jax.random.fold_in(jax.random.fold_in(own_key, 6), axis_at), (parts,), jnp.float32, low / len(cuts), largest / len(cuts))
        factor_of = factor_of * jnp.repeat(jnp.exp(draws), extent[axis_at] // parts).reshape((-1,) + (1,) * (len(extent) - 1 - axis_at))
    return factor_of


def rank_table(amount, slope):
    weights = [(1 << 20) // math.isqrt(standing ** slope) + 1 for standing in range(1, amount + 1)]
    scale = 1 + sum(weights) // (1 << 30)
    return np.cumsum(np.array([max(1, weight // scale) for weight in weights]))


def ranked_ids(stream_key, shape, count, slope):
    table = rank_table(count, slope)
    pick = jax.random.randint(jax.random.fold_in(stream_key, 1), shape, 0, int(table[count - 1]))
    standing = jnp.searchsorted(jnp.asarray(table, jnp.int32), pick, side="right")
    return jax.random.permutation(jax.random.fold_in(stream_key, 2), count)[standing].astype(jnp.int32)


def centred(key, dims, scale, reach, pieces=(), kind=jnp.bfloat16):
    values = scale * jax.random.normal(key, dims, jnp.float32)
    if pieces:
        values = values * steps_of(key, dims, pieces, -0.22, 0.18)
    return jnp.clip(values, -reach, reach).astype(kind)


def setup_inputs(seed: int = 0) -> dict:
    splits = jax.random.split(jax.random.key(seed), 10)
    hidden_act = draw_hidden_act(jax.random.fold_in(splits[9], 71), 0)
    down_weight = centred(splits[1], (FF, D), FF ** -0.5, 0.0625, ((0, 4),))
    residual = draw_residual(jax.random.fold_in(splits[9], 71), 0)
    post_gain = jnp.clip(1.0 + 0.18 * jax.random.normal(splits[3], (D,), jnp.float32), 0.1, 1.9)
    final_gain = jnp.clip(1.0 + 0.18 * jax.random.normal(splits[4], (D,), jnp.float32), 0.1, 1.9)
    vocab = draw_vocab(jax.random.fold_in(splits[9], 71), 0)
    vocab_bias = draw_vocab_bias(jax.random.fold_in(splits[9], 71), 0)
    target_ids = place_ends(ranked_ids(splits[7], (TOKENS, TOPK), V, 2), jax.random.fold_in(splits[7], 3), 0, V - 1).astype(jnp.int32)
    target_weights = draw_target_weights(jax.random.fold_in(splits[9], 71), 0)
    return dict(hidden_act=hidden_act, down_weight=down_weight, residual=residual, post_gain=post_gain, final_gain=final_gain, vocab=vocab, vocab_bias=vocab_bias, target_ids=target_ids, target_weights=target_weights)


epsilon = 1e-06
z_weight = 0.001
loss_scale = 32.0

def inverse_rms(values):
    return lax.rsqrt(lax.optimization_barrier(jnp.mean(values * values, axis=-1, keepdims=True)) + epsilon)

def reference(hidden_act, down_weight, residual, post_gain, final_gain, vocab, vocab_bias, target_ids, target_weights):
    branch = jnp.dot(hidden_act, down_weight, preferred_element_type=jnp.float32)
    stream = residual.astype(jnp.float32) + branch * inverse_rms(branch) * post_gain
    inverse = inverse_rms(stream)
    normed = (stream * inverse * final_gain).astype(jnp.bfloat16)
    columns = jnp.arange(V, dtype=jnp.int32)[None, :]

    def group(matrix_acc, inputs):
        row_block, target_block, weight_block = inputs
        scores = jnp.dot(row_block, vocab, preferred_element_type=jnp.float32) + vocab_bias
        row_max = lax.optimization_barrier(jnp.max(scores, axis=1))
        row_sum = lax.optimization_barrier(jnp.sum(jnp.exp(scores - row_max[:, None]), axis=1))
        log_norm = row_max + jnp.log(row_sum)
        wanted = jnp.zeros(scores.shape, jnp.float32)
        for target_k in range(TOPK):
            wanted = wanted + jnp.where(target_block[:, target_k:target_k + 1] == columns, weight_block[:, target_k:target_k + 1], 0.0)
        target_score = lax.optimization_barrier(jnp.sum(wanted * scores, axis=1))
        losses = log_norm - target_score + z_weight * log_norm * log_norm
        probability = jnp.exp(scores - log_norm[:, None])
        score_grads = (loss_scale * (probability * (1.0 + 2.0 * z_weight * log_norm)[:, None] - wanted)).astype(jnp.bfloat16)
        row_grad = lax.dot_general(score_grads, vocab, (((1,), (1,)), ((), ())), preferred_element_type=jnp.float32)
        matrix_acc = matrix_acc + lax.dot_general(row_block, score_grads, (((0,), (0,)), ((), ())), preferred_element_type=jnp.float32)
        return (matrix_acc, (losses, row_grad))
    stacked = (normed.reshape(N_DP, TOK_GRP, D), target_ids.reshape(N_DP, TOK_GRP, TOPK), target_weights.reshape(N_DP, TOK_GRP, TOPK))
    vocab_grad, outputs = lax.scan(group, jnp.zeros((D, V), jnp.float32), stacked)
    losses = outputs[0].reshape(TOKENS)
    row_grad = outputs[1].reshape(TOKENS, D)
    upstream = row_grad * final_gain
    stream_grad = inverse * (upstream - stream * inverse * inverse * lax.optimization_barrier(jnp.mean(upstream * stream, axis=-1, keepdims=True)))
    return (losses, stream_grad, vocab_grad)
```

```python
import jax
import jax.numpy as jnp
from jax import lax
from jax.sharding import PartitionSpec as P

CHUNKS = 4


epsilon = 1e-06
z_weight = 0.001
loss_scale = 32.0


def inverse_rms(values):
    return lax.rsqrt(jnp.mean(values * values, axis=-1, keepdims=True) + epsilon)


def shards(
    hidden_act,
    down_weight,
    residual,
    post_gain,
    final_gain,
    vocab,
    vocab_bias,
    target_ids,
    target_weights,
):
    own_rows = residual.shape[0]
    group_rows = hidden_act.shape[0]
    columns = vocab.shape[1]
    vp_index = lax.axis_index("vp")
    branch = lax.psum_scatter(
        jnp.dot(hidden_act, down_weight, preferred_element_type=jnp.float32),
        "vp",
        scatter_dimension=0,
        tiled=True,
    )
    stream = residual.astype(jnp.float32) + branch * inverse_rms(branch) * post_gain
    inverse = inverse_rms(stream)
    normed = (stream * inverse * final_gain).astype(jnp.bfloat16)
    gathered = lax.all_gather(normed, "vp", axis=0, tiled=True)
    local_ids = target_ids - vp_index * columns
    position = lax.broadcasted_iota(jnp.int32, (1, columns), 1)
    wanted = jnp.zeros((group_rows, columns), jnp.float32)
    for target_k in range(target_ids.shape[1]):
        wanted = wanted + jnp.where(
            local_ids[:, target_k : target_k + 1] == position,
            target_weights[:, target_k : target_k + 1],
            0.0,
        )
    scores = jnp.dot(gathered, vocab, preferred_element_type=jnp.float32) + vocab_bias[None, :]
    local_max = jnp.max(scores, axis=1)
    local_sum = jnp.sum(jnp.exp(scores - local_max[:, None]), axis=1)
    local_target = jnp.sum(wanted * scores, axis=1)
    stats = lax.all_gather(jnp.stack([local_max, local_sum, local_target]), "vp", axis=0)
    row_max = jnp.max(stats[:, 0], axis=0)
    row_sum = jnp.sum(stats[:, 1] * jnp.exp(stats[:, 0] - row_max), axis=0)
    target_score = jnp.sum(stats[:, 2], axis=0)
    log_norm = row_max + jnp.log(row_sum)
    group_losses = log_norm - target_score + z_weight * log_norm * log_norm
    losses = lax.dynamic_slice_in_dim(group_losses, vp_index * own_rows, own_rows, 0)
    factor = (1.0 + 2.0 * z_weight * log_norm)[:, None]
    probability = jnp.exp(scores - log_norm[:, None])
    score_grads = (loss_scale * (probability * factor - wanted)).astype(jnp.bfloat16)
    chunk = columns // CHUNKS
    pieces = []
    for index in range(CHUNKS):
        part = score_grads[:, index * chunk : (index + 1) * chunk]
        grad = lax.dot_general(
            gathered, part, (((0,), (0,)), ((), ())), preferred_element_type=jnp.float32
        ).astype(jnp.bfloat16)
        pieces.append(lax.psum_scatter(grad, "dp", scatter_dimension=0, tiled=True))
    row_grad = lax.psum_scatter(
        lax.dot_general(
            score_grads, vocab, (((1,), (1,)), ((), ())), preferred_element_type=jnp.float32
        ),
        "vp",
        scatter_dimension=0,
        tiled=True,
    )
    vocab_grad = jnp.concatenate([piece.astype(jnp.float32) for piece in pieces], axis=1)
    upstream = row_grad * final_gain
    stream_grad = inverse * (
        upstream - stream * inverse * inverse * jnp.mean(upstream * stream, axis=-1, keepdims=True)
    )
    return (losses, stream_grad, vocab_grad)


def solution(mesh):
    in_specs = (
        P("dp", "vp"),
        P("vp", None),
        P(("dp", "vp"), None),
        P(),
        P(),
        P(None, "vp"),
        P("vp"),
        P("dp", None),
        P("dp", None),
    )
    out_specs = (P(("dp", "vp")), P(("dp", "vp"), None), P("dp", "vp"))
    return jax.shard_map(shards, mesh=mesh, in_specs=in_specs, out_specs=out_specs, check_vma=False)
```
